32 devices in a mesh: sp: 8 (over z, y), tp: 4 (over x, core).
Axes of the slice: x: 2, y: 2, z: 4, core: 2. Of those that a mesh axis runs over, the one named last changes fastest.
Arguments:
- residual_input_stream: bfloat16 [6144, 2048], P('sp'), may hold values from -6 to 6
- projected_queries: bfloat16 [6144, 512], P('sp', 'tp'), may hold values from -6 to 6
- projected_keys: bfloat16 [6144, 512], P('sp', 'tp'), may hold values from -6 to 6
- projected_values: bfloat16 [6144, 1024], P('sp', 'tp'), may hold values from -6 to 6
- emitted_switch_entries: bfloat16 [6144, 1024], P('sp', 'tp'), may hold values from -6 to 6
- retention_preactivations: bfloat16 [6144, 512], P('sp', 'tp'), may hold values from -6 to 15
- additional_fading_amount: float32 [6144], P('sp'), may hold values from -2 to 0
- head_norm_gain: float32 [128], replicated, may hold values from 0.1 to 1.9
- attention_output_weight: bfloat16 [1024, 2048], P('tp'), may hold values from -0.1875 to 0.1875
- feedforward_norm_gain: float32 [2048], replicated, may hold values from 0.1 to 1.9
- gate_up_matrix: bfloat16 [2048, 5632], P('sp', 'tp'), may hold values from -0.125 to 0.125
- value_up_matrix: bfloat16 [2048, 5632], P('sp', 'tp'), may hold values from -0.125 to 0.125
- gate_filter_taps: bfloat16 [3, 5632], P(None, 'tp'), may hold values from -3.5 to 3.5
- value_filter_taps: bfloat16 [3, 5632], P(None, 'tp'), may hold values from -3.5 to 3.5
- down_projection_weight: bfloat16 [5632, 2048], P('tp', 'sp'), may hold values from -0.078125 to 0.078125
Outputs:
- layer_out: bfloat16 [6144, 2048], P(('sp', 'tp'))
The draws below stay inside these ranges and needn't reach their ends.
All inputs are finite; a program needn't handle non-finite values.
Results may differ from the reference program's by a relative error of at most 0.011.
Values may be sent and summed in bfloat16 or wider, within the bound.
A program may use at most 128 MiB of HBM per device.

```python
import math
import jax
import jax.numpy as jnp
from jax import lax

D = 2048
HEADS = 8
DK = 64
DV = 128
FF = 5632
CONV = 3
BLOCK = 64
TOK_DEV = 768
KW = 512
VW = 1024
TOKENS = 6144


def draw_retention_preactivations(key, part):
    keys_all = jax.random.split(jax.random.fold_in(key, 11), 3)
    ranking = jax.random.permutation(keys_all[0], HEADS)
    fast_count = HEADS // 2
    channel_head = jnp.arange(HEADS * DK) // DK
    head_fast = (ranking < fast_count).astype(jnp.float32)
    chan_fast = jnp.sum((channel_head[:, None] == jnp.arange(HEADS)[None, :]).astype(jnp.float32) * head_fast[None, :], axis=1)
    slow_base = math.log(TOKENS) - 1.6
    base = chan_fast + (1.0 - chan_fast) * slow_base
    device_count = TOKENS // TOK_DEV
    shifts = jax.random.uniform(keys_all[1], (device_count,), jnp.float32, -1.0, 1.0)
    position_dev = jnp.arange(TOKENS) // TOK_DEV
    shift_rows = jnp.sum((position_dev[:, None] == jnp.arange(device_count)[None, :]).astype(jnp.float32) * shifts[None, :], axis=1)
    noise = jnp.clip(jax.random.normal(keys_all[2], (TOKENS, HEADS * DK), jnp.float32), -5.0, 5.0)
    return (base[None, :] + shift_rows[:, None] + noise).astype(jnp.bfloat16)


def draw_additional_fading_amount(key, part):
    keys_all = jax.random.split(jax.random.fold_in(key, 23), 2)
    places = jax.random.randint(keys_all[0], (3,), 0, TOKENS)
    depths = jnp.log(jax.random.uniform(keys_all[1], (3,), jnp.float32, 0.5, 0.8))
    marks = (jnp.arange(TOKENS)[:, None] == places[None, :]).astype(jnp.float32)
    return jnp.sum(marks * depths[None, :], axis=1).astype(jnp.float32)


def levels(key, extent, shards, low, top_value):
    level = 1.0
    for position, parts in shards:
        steps = jax.random.uniform(jax.random.fold_in(jax.random.fold_in(key, 6), position), (parts,), jnp.float32, low / len(shards), top_value / len(shards))
        level = level * jnp.repeat(jnp.exp(steps), extent[position] // parts).reshape((-1,) + (1,) * (len(extent) - 1 - position))
    return level


def normal_values(stream_key, shape, scale, reach, pieces=(), kind=jnp.bfloat16):
    entries = jax.random.normal(stream_key, shape, jnp.float32) * scale
    if len(pieces) > 0:
        entries = levels(stream_key, shape, pieces, -0.22, 0.18) * entries
    return jnp.clip(entries, min=-reach, max=reach).astype(kind)


def setup_inputs(seed: int = 0) -> dict:
    seeds = jax.random.split(jax.random.key(seed), 16)
    residual_input_stream = normal_values(seeds[0], (TOKENS, D), 1.0, 6.0, ((0, 8),))
    projected_queries = normal_values(seeds[1], (TOKENS, KW), 1.0, 6.0, ((0, 8), (1, 4)))
    projected_keys = normal_values(seeds[2], (TOKENS, KW), 1.0, 6.0, ((0, 8), (1, 4)))
    projected_values = normal_values(seeds[3], (TOKENS, VW), 1.0, 6.0, ((0, 8), (1, 4)))
    emitted_switch_entries = normal_values(seeds[4], (TOKENS, VW), 1.0, 6.0, ((0, 8), (1, 4)))
    retention_preactivations = draw_retention_preactivations(jax.random.fold_in(seeds[15], 71), 0)
    additional_fading_amount = draw_additional_fading_amount(jax.random.fold_in(seeds[15], 71), 0)
    head_norm_gain = jnp.clip(1.0 + 0.18 * jax.random.normal(seeds[7], (DV,), jnp.float32), 0.1, 1.9)
    attention_output_weight = normal_values(seeds[8], (VW, D), VW ** -0.5, 0.1875, ((0, 4),))
    feedforward_norm_gain = jnp.clip(1.0 + 0.18 * jax.random.normal(seeds[9], (D,), jnp.float32), 0.1, 1.9)
    gate_up_matrix = normal_values(seeds[10], (D, FF), D ** -0.5, 0.125, ((0, 8), (1, 4)))
    value_up_matrix = normal_values(seeds[11], (D, FF), D ** -0.5, 0.125, ((0, 8), (1, 4)))
    gate_filter_taps = normal_values(seeds[12], (CONV, FF), CONV ** -0.5, 3.5, ((1, 4),))
    value_filter_taps = normal_values(seeds[13], (CONV, FF), CONV ** -0.5, 3.5, ((1, 4),))
    down_projection_weight = normal_values(seeds[14], (FF, D), FF ** -0.5, 0.078125, ((0, 4), (1, 8)))
    return dict(residual_input_stream=residual_input_stream, projected_queries=projected_queries, projected_keys=projected_keys, projected_values=projected_values, emitted_switch_entries=emitted_switch_entries, retention_preactivations=retention_preactivations, additional_fading_amount=additional_fading_amount, head_norm_gain=head_norm_gain, attention_output_weight=attention_output_weight, feedforward_norm_gain=feedforward_norm_gain, gate_up_matrix=gate_up_matrix, value_up_matrix=value_up_matrix, gate_filter_taps=gate_filter_taps, value_filter_taps=value_filter_taps, down_projection_weight=down_projection_weight)


eps = 1e-06
retention_sharpness = 16.0

def to_blocks(tensor, width):
    count = tensor.shape[0] // BLOCK
    return tensor.astype(jnp.float32).reshape(count, BLOCK, HEADS, width)

def depthwise(upward, taps):
    length = upward.shape[0]
    padded = jnp.concatenate([jnp.zeros((CONV - 1, upward.shape[1]), jnp.bfloat16), upward], axis=0)
    result = jnp.zeros(upward.shape, jnp.float32)
    for offset in range(CONV):
        result = result + taps[offset].astype(jnp.float32)[None] * padded[offset:offset + length].astype(jnp.float32)
    return result

def reference(residual_input_stream, projected_queries, projected_keys, projected_values, emitted_switch_entries, retention_preactivations, additional_fading_amount, head_norm_gain, attention_output_weight, feedforward_norm_gain, gate_up_matrix, value_up_matrix, gate_filter_taps, value_filter_taps, down_projection_weight):
    largest_exponent = lax.Precision.HIGHEST
    retention_logarithm = jax.nn.log_sigmoid(retention_preactivations.astype(jnp.float32)) / retention_sharpness + additional_fading_amount[:, None]
    scaled_q = to_blocks(projected_queries, DK) * DK ** (-0.5)
    key_heads = to_blocks(projected_keys, DK)
    value_heads = to_blocks(projected_values, DV)
    rate_cum = jnp.cumsum(to_blocks(retention_logarithm, DK), axis=1)
    block_total = rate_cum[:, -1]
    q_decayed = scaled_q * jnp.exp(rate_cum)
    k_growth = key_heads * jnp.exp(-rate_cum)
    fading_through_finish = key_heads * jnp.exp(block_total[:, None] - rate_cum)
    lower = jnp.tril(jnp.ones((BLOCK, BLOCK), bool))
    scores = jnp.einsum('nihk,njhk->nhij', q_decayed, k_growth, precision=largest_exponent)
    scores = jnp.where(lower[None, None], scores, 0.0)
    within = jnp.einsum('nhij,njhv->nihv', scores, value_heads, precision=largest_exponent)
    increments = jnp.einsum('nchk,nchv->nhkv', fading_through_finish, value_heads, precision=largest_exponent)

    def advance_recurrence(state, inputs):
        factor, increment = inputs
        return (factor[..., None] * state + increment, state)
    start_state = jnp.zeros((HEADS, DK, DV), jnp.float32)
    final_state, state_before = lax.scan(advance_recurrence, start_state, (jnp.exp(block_total), increments))
    earlier = jnp.einsum('nchk,nhkv->nchv', q_decayed, state_before, precision=largest_exponent)
    mech_out = (within + earlier).reshape(TOKENS, HEADS, DV)
    mech_out = mech_out * lax.rsqrt(lax.optimization_barrier(jnp.mean(mech_out * mech_out, axis=-1, keepdims=True)) + eps) * head_norm_gain
    mixed = (mech_out.reshape(TOKENS, VW) * jax.nn.silu(emitted_switch_entries.astype(jnp.float32))).astype(jnp.bfloat16)
    attended = jnp.dot(mixed, attention_output_weight, preferred_element_type=jnp.float32)
    resid = residual_input_stream.astype(jnp.float32) + attended
    normed = (resid * lax.rsqrt(lax.optimization_barrier(jnp.mean(resid * resid, axis=-1, keepdims=True)) + eps) * feedforward_norm_gain).astype(jnp.bfloat16)
    gate_up = jnp.dot(normed, gate_up_matrix, preferred_element_type=jnp.float32).astype(jnp.bfloat16)
    value_up = jnp.dot(normed, value_up_matrix, preferred_element_type=jnp.float32).astype(jnp.bfloat16)
    gate_mix = depthwise(gate_up, gate_filter_taps)
    value_mix = depthwise(value_up, value_filter_taps)
    hidden = (jax.nn.silu(gate_mix) * value_mix).astype(jnp.bfloat16)
    return (resid + jnp.dot(hidden, down_projection_weight, preferred_element_type=jnp.float32)).astype(jnp.bfloat16)
```

```python
import jax
import jax.numpy as jnp
from jax import lax
from jax.sharding import PartitionSpec as P

DK = 64
DV = 128
CONV = 3
BLOCK = 64
EDGE = 16


eps = 1e-06
retention_sharpness = 16.0


def from_behind(block, axis, distance):
    devices = range(lax.axis_size(axis))
    route = [(i - distance, i) for i in devices if i - distance in devices]
    return lax.ppermute(block, axis, route)


def to_blocks(tensor, local_heads, width):
    count = tensor.shape[0] // BLOCK
    return tensor.astype(jnp.float32).reshape(count, BLOCK, local_heads, width)


def row_norm(stream, gain):
    scaled = stream * lax.rsqrt(jnp.mean(stream * stream, axis=-1, keepdims=True) + eps)
    return (scaled * gain).astype(jnp.bfloat16)


def depthwise(padded, taps, length):
    start = padded.shape[0] - length - (CONV - 1)
    result = jnp.zeros((length, padded.shape[1]), jnp.float32)
    for offset in range(CONV):
        result = result + taps[offset].astype(jnp.float32)[None] * padded[
            start + offset : start + offset + length
        ].astype(jnp.float32)
    return result


def state_before_device(dev_log, dev_state):
    count, me = lax.axis_size("sp"), lax.axis_index("sp")
    heads, channels, width = dev_state.shape
    decay = jnp.broadcast_to(jnp.exp(dev_log)[..., None], (heads, channels, width))
    packed = jnp.concatenate([dev_state, decay], axis=0)
    arriving = jnp.zeros_like(dev_state)
    after = jnp.ones_like(dev_state)
    for distance in range(1, count):
        got = from_behind(packed, "sp", distance)
        arriving = arriving + after * got[:heads]
        after = after * got[heads:]
    return arriving


def xor_route(axis, bit):
    return [(i, i ^ bit) for i in range(lax.axis_size(axis))]


def ring_route(axis, step):
    count = lax.axis_size(axis)
    return [(i, (i + step) % count) for i in range(count)]


def exchange(block, axis, bit):
    return lax.ppermute(block, axis, xor_route(axis, bit))


def shifted(block, steps):
    return lax.ppermute(block, "sp", ring_route("sp", -2 * steps))


def ring_gather(block):
    pairs = lax.axis_size("sp") // 2
    held = [None] * pairs
    held[0] = block
    up = down = block
    for distance in range(1, pairs // 2 + 1):
        if 2 * distance < pairs:
            up = shifted(up, 1)
            down = shifted(down, -1)
            held[distance], held[pairs - distance] = up, down
        else:
            half = block.shape[0] // 2
            first = shifted(up[:half], 1)
            second = shifted(down[half:], -1)
            held[distance] = jnp.concatenate([first, second], axis=0)
    return held


def pair_then_ring(shard):
    me = lax.axis_index("sp")
    partner = exchange(shard, "sp", 1)
    own_first = me % 2 == 0
    both = jnp.stack(
        [jnp.where(own_first, shard, partner), jnp.where(own_first, partner, shard)]
    )
    flat = both.reshape((2 * shard.shape[0],) + shard.shape[1:])
    blocks = ring_gather(flat)
    pairs = len(blocks)
    full = jnp.zeros((pairs,) + flat.shape, flat.dtype)
    for distance, part in enumerate(blocks):
        full = lax.dynamic_update_index_in_dim(full, part, (me // 2 + distance) % pairs, 0)
    return full.reshape((pairs * flat.shape[0],) + flat.shape[1:])


def gather_tp(block):
    count, me = lax.axis_size("tp"), lax.axis_index("tp")
    held = block[None]
    bit = count // 2
    while bit:
        other = exchange(held, "tp", bit)
        low = (me & bit) == 0
        held = jnp.stack([jnp.where(low, held, other), jnp.where(low, other, held)])
        held = held.reshape((-1,) + block.shape)
        bit //= 2
    bits = count.bit_length() - 1
    order = [sum(((t >> b) & 1) << (bits - 1 - b) for b in range(bits)) for t in range(count)]
    return [held[o] for o in order]


def scatter_tp(partial):
    count, me = lax.axis_size("tp"), lax.axis_index("tp")
    rows = partial.shape[0] // count
    held = partial.reshape(count, rows, partial.shape[1])
    bit = 1
    while bit < count:
        mine = (me // bit) % 2
        split = held.reshape((-1, 2) + held.shape[1:])
        keep = lax.dynamic_index_in_dim(split, mine, 1, False)
        give = lax.dynamic_index_in_dim(split, 1 - mine, 1, False)
        got = exchange(give.astype(jnp.bfloat16), "tp", bit)
        held = keep.astype(jnp.float32) + got.astype(jnp.float32)
        bit *= 2
    return held[0]


def per_device(
    residual_input_stream,
    projected_queries,
    projected_keys,
    projected_values,
    emitted_switch_entries,
    retention_preactivations,
    additional_fading_amount,
    head_norm_gain,
    attention_output_weight,
    feedforward_norm_gain,
    gate_up_matrix,
    value_up_matrix,
    gate_filter_taps,
    value_filter_taps,
    down_projection_weight,
):
    largest_exponent = lax.Precision.HIGHEST
    tok_rows = residual_input_stream.shape[0]
    local_heads = projected_queries.shape[1] // DK
    gate_full = pair_then_ring(gate_up_matrix)
    value_full = pair_then_ring(value_up_matrix)
    down_near = ring_gather(down_projection_weight)
    down_far = [exchange(part, "sp", 1) for part in down_near]
    out_full = lax.all_gather(attention_output_weight, "tp", axis=0, tiled=True)
    retention_logarithm = (
        jax.nn.log_sigmoid(retention_preactivations.astype(jnp.float32)) / retention_sharpness
        + additional_fading_amount[:, None]
    )
    scaled_q = to_blocks(projected_queries, local_heads, DK) * DK ** (-0.5)
    key_heads = to_blocks(projected_keys, local_heads, DK)
    value_heads = to_blocks(projected_values, local_heads, DV)
    rate_cum = jnp.cumsum(to_blocks(retention_logarithm, local_heads, DK), axis=1)
    block_total = rate_cum[:, -1]
    before_block = jnp.cumsum(block_total, axis=0) - block_total
    q_decayed = scaled_q * jnp.exp(rate_cum)
    k_growth = key_heads * jnp.exp(-rate_cum)
    fading_through_finish = key_heads * jnp.exp(block_total[:, None] - rate_cum)
    lower = jnp.tril(jnp.ones((BLOCK, BLOCK), bool))
    scores = jnp.einsum("nihk,njhk->nhij", q_decayed, k_growth, precision=largest_exponent)
    scores = jnp.where(lower[None, None], scores, 0.0)
    within = jnp.einsum("nhij,njhv->nihv", scores, value_heads, precision=largest_exponent)
    increments = jnp.einsum(
        "nchk,nchv->nhkv", fading_through_finish, value_heads, precision=largest_exponent
    )

    def advance_recurrence(state, inputs):
        factor, increment = inputs
        return (factor[..., None] * state + increment, state)

    start_state = jnp.zeros((local_heads, DK, DV), jnp.float32)
    dev_state, state_before = lax.scan(
        advance_recurrence, start_state, (jnp.exp(block_total), increments)
    )
    earlier = jnp.einsum("nchk,nhkv->nchv", q_decayed, state_before, precision=largest_exponent)
    query_shard = scaled_q * jnp.exp(rate_cum + before_block[:, None])
    dev_log = jnp.sum(block_total, axis=0)

    arriving_state = state_before_device(dev_log, dev_state)
    earlier_memory_share = jnp.einsum(
        "osyq,yqi->osyi", query_shard, arriving_state, precision=largest_exponent
    )
    mech_out = (within + earlier + earlier_memory_share).reshape(tok_rows, local_heads, DV)
    mech_out = (
        mech_out
        * lax.rsqrt(jnp.mean(mech_out * mech_out, axis=-1, keepdims=True) + eps)
        * head_norm_gain
    )
    mixed = (
        mech_out.reshape(tok_rows, local_heads * DV)
        * jax.nn.silu(emitted_switch_entries.astype(jnp.float32))
    ).astype(jnp.bfloat16)
    sp_count, sp_index = (lax.axis_size("sp"), lax.axis_index("sp"))
    tp_count, tp_index = (lax.axis_size("tp"), lax.axis_index("tp"))
    share = tok_rows // tp_count
    mixed_all = jnp.concatenate(gather_tp(mixed), axis=1)
    attended = jnp.dot(mixed_all, out_full, preferred_element_type=jnp.float32)
    resid = residual_input_stream.astype(jnp.float32) + attended
    normed = row_norm(resid, feedforward_norm_gain)
    resid_own = lax.dynamic_slice_in_dim(resid, tp_index * share, share, 0)
    tail = from_behind(normed[tok_rows - EDGE :], "sp", 1)
    rows = jnp.concatenate([tail, normed], axis=0)
    gate_up = jnp.dot(rows, gate_full, preferred_element_type=jnp.float32).astype(jnp.bfloat16)
    value_up = jnp.dot(rows, value_full, preferred_element_type=jnp.float32).astype(jnp.bfloat16)
    gate_mix = depthwise(gate_up, gate_filter_taps, tok_rows)
    value_mix = depthwise(value_up, value_filter_taps, tok_rows)
    hidden = (jax.nn.silu(gate_mix) * value_mix).astype(jnp.bfloat16)
    pairs = sp_count // 2
    width = down_projection_weight.shape[1]
    feed = jnp.zeros((sp_count, share, width), jnp.float32)
    for distance in sorted(range(pairs), key=lambda d: min(d, pairs - d)):
        both = jnp.concatenate([down_near[distance], down_far[distance]], axis=1)
        partial = jnp.dot(hidden, both, preferred_element_type=jnp.float32)
        summed = scatter_tp(partial)
        place = (sp_index // 2 + distance) % pairs * 2
        feed = lax.dynamic_update_index_in_dim(feed, summed[:, :width], place + sp_index % 2, 0)
        feed = lax.dynamic_update_index_in_dim(feed, summed[:, width:], place + 1 - sp_index % 2, 0)
    feed = feed.transpose(1, 0, 2).reshape(share, sp_count * width)
    return (resid_own + feed).astype(jnp.bfloat16)


def solution(mesh):
    placed = (
        P("sp", None),
        P("sp", "tp"),
        P("sp", "tp"),
        P("sp", "tp"),
        P("sp", "tp"),
        P("sp", "tp"),
        P("sp"),
        P(),
        P("tp", None),
        P(),
        P("sp", "tp"),
        P("sp", "tp"),
        P(None, "tp"),
        P(None, "tp"),
        P("tp", "sp"),
    )
    return jax.shard_map(
        per_device, mesh=mesh, in_specs=placed, out_specs=P(("sp", "tp"), None), check_vma=False
    )
```

```python
import jax
import jax.numpy as jnp
from jax import lax
from jax.sharding import Mesh, PartitionSpec as P

DK = 64
DV = 128
CONV = 3
BLOCK = 64
EDGE = 16
SP = ("so", "si")


eps = 1e-06
retention_sharpness = 16.0


def from_behind(block, axis, distance):
    devices = range(lax.axis_size(axis))
    route = [(i - distance, i) for i in devices if i - distance in devices]
    return lax.ppermute(block, axis, route)


def to_blocks(tensor, local_heads, width):
    count = tensor.shape[0] // BLOCK
    return tensor.astype(jnp.float32).reshape(count, BLOCK, local_heads, width)


def row_norm(stream, gain):
    scaled = stream * lax.rsqrt(jnp.mean(stream * stream, axis=-1, keepdims=True) + eps)
    return (scaled * gain).astype(jnp.bfloat16)


def depthwise(padded, taps, length):
    start = padded.shape[0] - length - (CONV - 1)
    result = jnp.zeros((length, padded.shape[1]), jnp.float32)
    for offset in range(CONV):
        result = result + taps[offset].astype(jnp.float32)[None] * padded[
            start + offset : start + offset + length
        ].astype(jnp.float32)
    return result


def state_before_device(dev_log, dev_state):
    heads, channels, width = dev_state.shape
    lanes = heads * channels
    decay = jnp.pad(jnp.exp(dev_log).reshape(1, lanes), ((0, 0), (0, -lanes % width)))
    decay = decay.reshape(-1, width)
    packed = jnp.concatenate([dev_state.reshape(lanes, width), decay], axis=0)
    arriving = jnp.zeros_like(dev_state)
    after = jnp.ones((heads, channels), jnp.float32)
    for distance in range(1, lax.axis_size("so") * lax.axis_size("si")):
        got = from_behind(packed, SP, distance)
        arriving = arriving + after[..., None] * got[:lanes].reshape(dev_state.shape)
        after = after * got[lanes:].reshape(-1)[:lanes].reshape(after.shape)
    return arriving


def xor_route(axis, bit):
    return [(i, i ^ bit) for i in range(lax.axis_size(axis))]


def ring_route(axis, step):
    count = lax.axis_size(axis)
    return [(i, (i + step) % count) for i in range(count)]


def exchange(block, axis, bit):
    return lax.ppermute(block, axis, xor_route(axis, bit))


def in_order(own, other, axis, dim):
    first = lax.axis_index(axis) % 2 == 0
    return jnp.concatenate([jnp.where(first, own, other), jnp.where(first, other, own)], axis=dim)


def gather_tp(block):
    count, me = lax.axis_size("tp"), lax.axis_index("tp")
    held = block[None]
    bit = count // 2
    while bit:
        other = exchange(held, "tp", bit)
        low = (me & bit) == 0
        held = jnp.stack([jnp.where(low, held, other), jnp.where(low, other, held)])
        held = held.reshape((-1,) + block.shape)
        bit //= 2
    bits = count.bit_length() - 1
    order = [sum(((t >> b) & 1) << (bits - 1 - b) for b in range(bits)) for t in range(count)]
    return [held[o] for o in order]


def split_columns(rows, width):
    first = lax.axis_index("si") == 0
    pieces = [rows[:, i : i + width] for i in range(0, rows.shape[1], width)]
    even, odd = pieces[::2], pieces[1::2]
    near = [jnp.where(first, e, o) for e, o in zip(even, odd)]
    far = [jnp.where(first, o, e) for e, o in zip(even, odd)]
    return jnp.concatenate(near, axis=1), jnp.concatenate(far, axis=1)


def two_part(near, far, line):
    partner = exchange(line, "si", 1)
    total = jnp.dot(near, line, preferred_element_type=jnp.float32)
    total = total + jnp.dot(far, partner, preferred_element_type=jnp.float32)
    return total.astype(jnp.bfloat16)


def scatter_tp(partial):
    count, me = lax.axis_size("tp"), lax.axis_index("tp")
    rows = partial.shape[0] // count
    held = partial.reshape(count, rows, partial.shape[1])
    bit = 1
    while bit < count:
        mine = (me // bit) % 2
        split = held.reshape((-1, 2) + held.shape[1:])
        keep = lax.dynamic_index_in_dim(split, mine, 1, False)
        give = lax.dynamic_index_in_dim(split, 1 - mine, 1, False)
        got = exchange(give.astype(jnp.bfloat16), "tp", bit)
        held = keep.astype(jnp.float32) + got.astype(jnp.float32)
        bit *= 2
    return held[0]


def per_device(
    residual_input_stream,
    projected_queries,
    projected_keys,
    projected_values,
    emitted_switch_entries,
    retention_preactivations,
    additional_fading_amount,
    head_norm_gain,
    attention_output_weight,
    feedforward_norm_gain,
    gate_up_matrix,
    value_up_matrix,
    gate_filter_taps,
    value_filter_taps,
    down_projection_weight,
):
    largest_exponent = lax.Precision.HIGHEST
    tok_rows = residual_input_stream.shape[0]
    local_heads = projected_queries.shape[1] // DK
    gate_line = lax.all_gather(gate_up_matrix, "so", axis=0, tiled=True)
    value_line = lax.all_gather(value_up_matrix, "so", axis=0, tiled=True)
    down_other = exchange(down_projection_weight, "si", 1)
    down_pair = in_order(down_projection_weight, down_other, "si", 1)
    down_line = lax.all_gather(down_pair, "so", axis=0)
    out_full = jnp.concatenate(gather_tp(attention_output_weight), axis=0)
    retention_logarithm = (
        jax.nn.log_sigmoid(retention_preactivations.astype(jnp.float32)) / retention_sharpness
        + additional_fading_amount[:, None]
    )
    scaled_q = to_blocks(projected_queries, local_heads, DK) * DK ** (-0.5)
    key_heads = to_blocks(projected_keys, local_heads, DK)
    value_heads = to_blocks(projected_values, local_heads, DV)
    rate_cum = jnp.cumsum(to_blocks(retention_logarithm, local_heads, DK), axis=1)
    block_total = rate_cum[:, -1]
    before_block = jnp.cumsum(block_total, axis=0) - block_total
    q_decayed = scaled_q * jnp.exp(rate_cum)
    k_growth = key_heads * jnp.exp(-rate_cum)
    fading_through_finish = key_heads * jnp.exp(block_total[:, None] - rate_cum)
    lower = jnp.tril(jnp.ones((BLOCK, BLOCK), bool))
    scores = jnp.einsum("nihk,njhk->nhij", q_decayed, k_growth, precision=largest_exponent)
    scores = jnp.where(lower[None, None], scores, 0.0)
    within = jnp.einsum("nhij,njhv->nihv", scores, value_heads, precision=largest_exponent)
    increments = jnp.einsum(
        "nchk,nchv->nhkv", fading_through_finish, value_heads, precision=largest_exponent
    )

    count = block_total.shape[0]
    ends = before_block + block_total
    reached = jnp.concatenate([before_block, ends[-1:]], axis=0)
    earlier_block = jnp.arange(count)[None, :] < jnp.arange(count + 1)[:, None]
    fade = jnp.where(
        earlier_block[..., None, None],
        jnp.exp(jnp.minimum(reached[:, None] - ends[None], 0.0)),
        0.0,
    )
    states = jnp.sum(fade[..., None] * increments[None], axis=1)
    state_before, dev_state = states[:-1], states[-1]
    earlier = jnp.einsum("nchk,nhkv->nchv", q_decayed, state_before, precision=largest_exponent)
    query_shard = scaled_q * jnp.exp(rate_cum + before_block[:, None])
    dev_log = jnp.sum(block_total, axis=0)

    arriving_state = state_before_device(dev_log, dev_state)
    earlier_memory_share = jnp.einsum(
        "osyq,yqi->osyi", query_shard, arriving_state, precision=largest_exponent
    )
    mech_out = (within + earlier + earlier_memory_share).reshape(tok_rows, local_heads, DV)
    mech_out = (
        mech_out
        * lax.rsqrt(jnp.mean(mech_out * mech_out, axis=-1, keepdims=True) + eps)
        * head_norm_gain
    )
    mixed = (
        mech_out.reshape(tok_rows, local_heads * DV)
        * jax.nn.silu(emitted_switch_entries.astype(jnp.float32))
    ).astype(jnp.bfloat16)
    tp_count, tp_index = (lax.axis_size("tp"), lax.axis_index("tp"))
    share = tok_rows // tp_count
    mixed_all = jnp.concatenate(gather_tp(mixed), axis=1)
    attended = jnp.dot(mixed_all, out_full, preferred_element_type=jnp.float32)
    resid = residual_input_stream.astype(jnp.float32) + attended
    normed = row_norm(resid, feedforward_norm_gain)
    resid_own = lax.dynamic_slice_in_dim(resid, tp_index * share, share, 0)
    tail = from_behind(normed[tok_rows - EDGE :], SP, 1)
    rows = jnp.concatenate([tail, normed], axis=0)
    near, far = split_columns(rows, gate_up_matrix.shape[0])
    gate_up = two_part(near, far, gate_line)
    value_up = two_part(near, far, value_line)
    gate_mix = depthwise(gate_up, gate_filter_taps, tok_rows)
    value_mix = depthwise(value_up, value_filter_taps, tok_rows)
    hidden = (jax.nn.silu(gate_mix) * value_mix).astype(jnp.bfloat16)
    feed = jnp.concatenate(
        [
            scatter_tp(jnp.dot(hidden, part, preferred_element_type=jnp.float32))
            for part in down_line
        ],
        axis=1,
    )
    return (resid_own + feed).astype(jnp.bfloat16)


def solution(mesh):
    sp, tp = mesh.shape["sp"], mesh.shape["tp"]
    split = Mesh(mesh.devices.reshape(sp // 2, 2, tp), ("so", "si", "tp"))
    placed = (
        P(SP, None),
        P(SP, "tp"),
        P(SP, "tp"),
        P(SP, "tp"),
        P(SP, "tp"),
        P(SP, "tp"),
        P(SP),
        P(),
        P("tp", None),
        P(),
        P(SP, "tp"),
        P(SP, "tp"),
        P(None, "tp"),
        P(None, "tp"),
        P("tp", SP),
    )
    return jax.shard_map(
        per_device, mesh=split, in_specs=placed, out_specs=P(("so", "si", "tp"), None), check_vma=False
    )
```

```python
import jax
import jax.numpy as jnp
from jax import lax
from jax.sharding import Mesh, PartitionSpec as P

DK = 64
DV = 128
CONV = 3
BLOCK = 64
EDGE = 16
SP = ("so", "si")


eps = 1e-06
retention_sharpness = 16.0


def from_behind(block, axis, distance):
    devices = range(lax.axis_size(axis))
    route = [(i - distance, i) for i in devices if i - distance in devices]
    return lax.ppermute(block, axis, route)


def to_blocks(tensor, local_heads, width):
    count = tensor.shape[0] // BLOCK
    return tensor.astype(jnp.float32).reshape(count, BLOCK, local_heads, width)


def row_norm(stream, gain):
    scaled = stream * lax.rsqrt(jnp.mean(stream * stream, axis=-1, keepdims=True) + eps)
    return (scaled * gain).astype(jnp.bfloat16)


def depthwise(padded, taps, length):
    start = padded.shape[0] - length - (CONV - 1)
    result = jnp.zeros((length, padded.shape[1]), jnp.float32)
    for offset in range(CONV):
        result = result + taps[offset].astype(jnp.float32)[None] * padded[
            start + offset : start + offset + length
        ].astype(jnp.float32)
    return result


def state_before_device(dev_log, dev_state):
    heads, channels, width = dev_state.shape
    lanes = heads * channels
    decay = jnp.pad(jnp.exp(dev_log).reshape(1, lanes), ((0, 0), (0, -lanes % width)))
    decay = decay.reshape(-1, width)
    packed = jnp.concatenate([dev_state.reshape(lanes, width), decay], axis=0)
    arriving = jnp.zeros_like(dev_state)
    after = jnp.ones((heads, channels), jnp.float32)
    for distance in range(1, lax.axis_size("so") * lax.axis_size("si")):
        got = from_behind(packed, SP, distance)
        arriving = arriving + after[..., None] * got[:lanes].reshape(dev_state.shape)
        after = after * got[lanes:].reshape(-1)[:lanes].reshape(after.shape)
    return arriving


def xor_route(axis, bit):
    return [(i, i ^ bit) for i in range(lax.axis_size(axis))]


def ring_route(axis, step):
    count = lax.axis_size(axis)
    return [(i, (i + step) % count) for i in range(count)]


def exchange(block, axis, bit):
    return lax.ppermute(block, axis, xor_route(axis, bit))


def in_order(own, other, axis, dim):
    first = lax.axis_index(axis) % 2 == 0
    return jnp.concatenate([jnp.where(first, own, other), jnp.where(first, other, own)], axis=dim)


def gather_tp(block):
    count, me = lax.axis_size("tp"), lax.axis_index("tp")
    held = block[None]
    bit = count // 2
    while bit:
        other = exchange(held, "tp", bit)
        low = (me & bit) == 0
        held = jnp.stack([jnp.where(low, held, other), jnp.where(low, other, held)])
        held = held.reshape((-1,) + block.shape)
        bit //= 2
    bits = count.bit_length() - 1
    order = [sum(((t >> b) & 1) << (bits - 1 - b) for b in range(bits)) for t in range(count)]
    return [held[o] for o in order]


def split_columns(rows, width):
    first = lax.axis_index("si") == 0
    pieces = [rows[:, i : i + width] for i in range(0, rows.shape[1], width)]
    even, odd = pieces[::2], pieces[1::2]
    near = [jnp.where(first, e, o) for e, o in zip(even, odd)]
    far = [jnp.where(first, o, e) for e, o in zip(even, odd)]
    return jnp.concatenate(near, axis=1), jnp.concatenate(far, axis=1)


def two_part(near, far, line):
    partner = exchange(line, "si", 1)
    total = jnp.dot(near, line, preferred_element_type=jnp.float32)
    total = total + jnp.dot(far, partner, preferred_element_type=jnp.float32)
    return total.astype(jnp.bfloat16)


def scatter_tp(partial):
    count, me = lax.axis_size("tp"), lax.axis_index("tp")
    rows = partial.shape[0] // count
    held = partial.reshape(count, rows, partial.shape[1])
    bit = 1
    while bit < count:
        mine = (me // bit) % 2
        split = held.reshape((-1, 2) + held.shape[1:])
        keep = lax.dynamic_index_in_dim(split, mine, 1, False)
        give = lax.dynamic_index_in_dim(split, 1 - mine, 1, False)
        got = exchange(give.astype(jnp.bfloat16), "tp", bit)
        held = keep.astype(jnp.float32) + got.astype(jnp.float32)
        bit *= 2
    return held[0]


def per_device(
    residual_input_stream,
    projected_queries,
    projected_keys,
    projected_values,
    emitted_switch_entries,
    retention_preactivations,
    additional_fading_amount,
    head_norm_gain,
    attention_output_weight,
    feedforward_norm_gain,
    gate_up_matrix,
    value_up_matrix,
    gate_filter_taps,
    value_filter_taps,
    down_projection_weight,
):
    largest_exponent = lax.Precision.HIGHEST
    tok_rows = residual_input_stream.shape[0]
    local_heads = projected_queries.shape[1] // DK
    gate_line = lax.all_gather(gate_up_matrix, "so", axis=0, tiled=True)
    value_line = lax.all_gather(value_up_matrix, "so", axis=0, tiled=True)
    down_other = exchange(down_projection_weight, "si", 1)
    down_pair = in_order(down_projection_weight, down_other, "si", 1)
    half = down_pair.shape[1] // 2
    down_first = lax.all_gather(down_pair[:, :half], "so", axis=0)
    down_second = lax.all_gather(down_pair[:, half:], "so", axis=0)
    out_full = jnp.concatenate(gather_tp(attention_output_weight), axis=0)
    retention_logarithm = (
        jax.nn.log_sigmoid(retention_preactivations.astype(jnp.float32)) / retention_sharpness
        + additional_fading_amount[:, None]
    )
    scaled_q = to_blocks(projected_queries, local_heads, DK) * DK ** (-0.5)
    key_heads = to_blocks(projected_keys, local_heads, DK)
    value_heads = to_blocks(projected_values, local_heads, DV)
    rate_cum = jnp.cumsum(to_blocks(retention_logarithm, local_heads, DK), axis=1)
    block_total = rate_cum[:, -1]
    before_block = jnp.cumsum(block_total, axis=0) - block_total
    q_decayed = scaled_q * jnp.exp(rate_cum)
    k_growth = key_heads * jnp.exp(-rate_cum)
    fading_through_finish = key_heads * jnp.exp(block_total[:, None] - rate_cum)
    lower = jnp.tril(jnp.ones((BLOCK, BLOCK), bool))
    scores = jnp.einsum("nihk,njhk->nhij", q_decayed, k_growth, precision=largest_exponent)
    scores = jnp.where(lower[None, None], scores, 0.0)
    within = jnp.einsum("nhij,njhv->nihv", scores, value_heads, precision=largest_exponent)
    increments = jnp.einsum(
        "nchk,nchv->nhkv", fading_through_finish, value_heads, precision=largest_exponent
    )

    count = block_total.shape[0]
    ends = before_block + block_total
    reached = jnp.concatenate([before_block, ends[-1:]], axis=0)
    earlier_block = jnp.arange(count)[None, :] < jnp.arange(count + 1)[:, None]
    fade = jnp.where(
        earlier_block[..., None, None],
        jnp.exp(jnp.minimum(reached[:, None] - ends[None], 0.0)),
        0.0,
    )
    states = jnp.sum(fade[..., None] * increments[None], axis=1)
    state_before, dev_state = states[:-1], states[-1]
    earlier = jnp.einsum("nchk,nhkv->nchv", q_decayed, state_before, precision=largest_exponent)
    query_shard = scaled_q * jnp.exp(rate_cum + before_block[:, None])
    dev_log = jnp.sum(block_total, axis=0)

    arriving_state = state_before_device(dev_log, dev_state)
    earlier_memory_share = jnp.einsum(
        "osyq,yqi->osyi", query_shard, arriving_state, precision=largest_exponent
    )
    mech_out = (within + earlier + earlier_memory_share).reshape(tok_rows, local_heads, DV)
    mech_out = (
        mech_out
        * lax.rsqrt(jnp.mean(mech_out * mech_out, axis=-1, keepdims=True) + eps)
        * head_norm_gain
    )
    mixed = (
        mech_out.reshape(tok_rows, local_heads * DV)
        * jax.nn.silu(emitted_switch_entries.astype(jnp.float32))
    ).astype(jnp.bfloat16)
    tp_count, tp_index = (lax.axis_size("tp"), lax.axis_index("tp"))
    share = tok_rows // tp_count
    mixed_all = jnp.concatenate(gather_tp(mixed), axis=1)
    attended = jnp.dot(mixed_all, out_full, preferred_element_type=jnp.float32)
    resid = residual_input_stream.astype(jnp.float32) + attended
    normed = row_norm(resid, feedforward_norm_gain)
    resid_own = lax.dynamic_slice_in_dim(resid, tp_index * share, share, 0)
    tail = from_behind(normed[tok_rows - EDGE :], SP, 1)
    rows = jnp.concatenate([tail, normed], axis=0)
    value_line, rows = lax.optimization_barrier((value_line, rows))
    near, far = split_columns(rows, gate_up_matrix.shape[0])
    gate_up = two_part(near, far, gate_line)
    value_up = two_part(near, far, value_line)
    gate_mix = depthwise(gate_up, gate_filter_taps, tok_rows)
    value_mix = depthwise(value_up, value_filter_taps, tok_rows)
    hidden = (jax.nn.silu(gate_mix) * value_mix).astype(jnp.bfloat16)
    firsts, seconds = (
        scatter_tp(
            jnp.concatenate(
                [jnp.dot(hidden, part, preferred_element_type=jnp.float32) for part in line],
                axis=1,
            )
        )
        for line in (down_first, down_second)
    )
    starts = range(0, firsts.shape[1], half)
    feed = jnp.concatenate(
        [piece[:, i : i + half] for i in starts for piece in (firsts, seconds)], axis=1
    )
    return (resid_own + feed).astype(jnp.bfloat16)


def solution(mesh):
    sp, tp = mesh.shape["sp"], mesh.shape["tp"]
    split = Mesh(mesh.devices.reshape(sp // 2, 2, tp), ("so", "si", "tp"))
    placed = (
        P(SP, None),
        P(SP, "tp"),
        P(SP, "tp"),
        P(SP, "tp"),
        P(SP, "tp"),
        P(SP, "tp"),
        P(SP),
        P(),
        P("tp", None),
        P(),
        P(SP, "tp"),
        P(SP, "tp"),
        P(None, "tp"),
        P(None, "tp"),
        P("tp", SP),
    )
    return jax.shard_map(
        per_device, mesh=split, in_specs=placed, out_specs=P(("so", "si", "tp"), None), check_vma=False
    )
```
